32 devices in a mesh: grp: 2 (over x), ep: 16 (over z, y, core).
Axes of the slice: x: 2, y: 2, z: 4, core: 2. Of those that a mesh axis runs over, the one named last changes fastest.
Arguments:
- tokens: bfloat16 [4096, 2048], P(('grp', 'ep')), parts along dimension 0, may hold values from -6 to 6
- norm_gain: float32 [2048], replicated, may hold values from 0.1 to 1.9
- expert_ids: int32 [4096, 2], P(('grp', 'ep')), parts along dimension 0, may hold values from 0 to 3, as said below
- mix_weights: float32 [4096, 2], P(('grp', 'ep')), parts along dimension 0, may hold values from 0.2 to 1
- gate_weight: bfloat16 [2048, 28672], P(None, 'ep'), may hold values from -0.125 to 0.125
- up_weight: bfloat16 [2048, 28672], P(None, 'ep'), may hold values from -0.125 to 0.125
- down_weight: bfloat16 [28672, 2048], P('ep'), may hold values from -0.0625 to 0.0625
Outputs:
- mixed: bfloat16 [4096, 2048], P(('grp', 'ep')), parts along dimension 0
The draws below stay inside these ranges and needn't reach their ends.
There are 2 independent parts, one for each index of `grp`. The reference program is written for one: setup_inputs(seed, part) draws one part's arguments, and reference() takes and returns one part's arrays. A program takes and returns all parts, laid end to end along the dimension named above; an argument that names none is the same for every part. Nothing has to cross between parts.
Inputs may be any that keep to these rules, and one draw needn't show every extreme that they name: `expert_ids`: each token names 2 different experts. In the rows of one device no expert is named by more than 80 rows, and in every draw each expert is named by exactly 80 rows of some device.
All inputs are finite; a program needn't handle non-finite values.
Results may differ from the reference program's by a relative error of at most 0.008.
Values may be sent and summed in bfloat16 or wider, within the bound.
No kernel may reach another device: no remote copies, remote signals or barrier semaphores. Data moves between devices by JAX's collectives and lax.ppermute only.
A program may use at most 128 MiB of HBM per device.

```python
import jax
import jax.numpy as jnp
from jax import lax

D = 2048
FF = 7168
TOP = 2
SPLIT = 4
TOK_DEV = 128
EXPERTS = 4
CAP = 80
TOKENS = 2048
N_EP = 16


def draw_expert_ids(key, part):
    key_shift = jax.random.fold_in(key, 11)
    key_offset = jax.random.fold_in(key, 12)
    key_order = jax.random.fold_in(key, 13)
    key_swap = jax.random.fold_in(key, 14)
    shift = jax.random.randint(key_shift, (), 0, EXPERTS)
    blocks = jnp.arange(N_EP, dtype=jnp.int32)
    favoured = ((blocks + shift) % EXPERTS)[:, None]
    positions = jnp.arange(TOK_DEV, dtype=jnp.int32)
    chosen = positions < CAP
    picks_before = jnp.where(chosen, positions, CAP + 2 * (positions - CAP))[None, :]
    offsets = jax.random.randint(key_offset, (N_EP, 1), 0, EXPERTS - 1)
    first_other = (picks_before + offsets) % (EXPERTS - 1)
    second_other = (picks_before + 1 + offsets) % (EXPERTS - 1)
    first_expert = (favoured + 1 + first_other) % EXPERTS
    second_expert = (favoured + 1 + second_other) % EXPERTS
    column_one = jnp.where(chosen[None, :], favoured, first_expert)
    column_two = jnp.where(chosen[None, :], first_expert, second_expert)
    orders = jax.vmap(lambda k: jax.random.permutation(k, TOK_DEV))(jax.random.split(key_order, N_EP))
    column_one = jnp.take_along_axis(column_one, orders, axis=1)
    column_two = jnp.take_along_axis(column_two, orders, axis=1)
    flips = jax.random.randint(key_swap, (N_EP, TOK_DEV), 0, 2)
    left = jnp.where(flips == 1, column_two, column_one)
    right = jnp.where(flips == 1, column_one, column_two)
    paired = jnp.stack([left, right], axis=2)
    return paired.reshape(TOKENS, TOP).astype(jnp.int32)


def steps_of(own_key, extent, shards, low, high):
    level = 1.0
    for position, shards_of in shards:
        heights = jax.random.uniform(jax.random.fold_in(jax.random.fold_in(own_key, 6), position), (shards_of,), jnp.float32, low / len(shards), high / len(shards))
        level = level * jnp.repeat(jnp.exp(heights), extent[position] // shards_of).reshape((-1,) + (1,) * (len(extent) - 1 - position))
    return level


def scatter_about(stream_key, dims, spread, most, pieces=(), kind=jnp.bfloat16):
    entries = spread * jax.random.normal(stream_key, dims, jnp.float32)
    if pieces:
        entries = entries * steps_of(stream_key, dims, pieces, -0.22, 0.18)
    return jnp.clip(entries, -most, most).astype(kind)


def setup_inputs(seed: int = 0, part: int = 0) -> dict:
    key_of = jax.random.split(jax.random.key(seed), 8)
    own_keys = jax.random.split(jax.random.fold_in(key_of[7], part), 8)
    return {
        "tokens": scatter_about(own_keys[0], (TOKENS, D), 1.0, 6.0, ((0, 16),)),
        "norm_gain": jnp.clip(1.0 + 0.18 * jax.random.normal(key_of[1], (D,), jnp.float32), 0.1, 1.9),
        "expert_ids": draw_expert_ids(jax.random.fold_in(jax.random.fold_in(key_of[7], part), 71), part),
        "mix_weights": jnp.clip(0.2 + 0.8 * jax.random.uniform(own_keys[3], (TOKENS, TOP), jnp.float32) ** steps_of(own_keys[3], (TOKENS, TOP), ((0, 16),), -0.2, 0.2), 0.2, 1.0),
        "gate_weight": scatter_about(key_of[4], (D, EXPERTS * FF), D ** -0.5, 0.125, ((1, 16),)),
        "up_weight": scatter_about(key_of[5], (D, EXPERTS * FF), D ** -0.5, 0.125, ((1, 16),)),
        "down_weight": scatter_about(key_of[6], (EXPERTS * FF, D), FF ** -0.5, 0.0625, ((0, 16),)),
    }


def block_slots(ids):
    flat = ids.reshape(-1)
    onehot = (flat[:, None] == jnp.arange(EXPERTS, dtype=jnp.int32)[None, :]).astype(jnp.int32)
    before = jnp.cumsum(onehot, axis=0) - onehot
    return lax.optimization_barrier(jnp.sum(before * onehot, axis=1)).reshape(ids.shape)

def reference(tokens, norm_gain, expert_ids, mix_weights, gate_weight, up_weight, down_weight):
    values = tokens.astype(jnp.float32)
    normed = (values * lax.rsqrt(lax.optimization_barrier(jnp.mean(values * values, axis=-1, keepdims=True)) + 1e-06) * norm_gain).astype(jnp.bfloat16)
    ids = expert_ids.reshape(N_EP, TOK_DEV, TOP)
    slots = jax.vmap(block_slots)(ids)
    source = jnp.broadcast_to(jnp.arange(N_EP, dtype=jnp.int32)[:, None, None], ids.shape)
    rows = jnp.broadcast_to(normed.reshape(N_EP, TOK_DEV, 1, D), (N_EP, TOK_DEV, TOP, D))
    buffers = jnp.zeros((EXPERTS, N_EP, CAP, D), jnp.bfloat16)
    buffers = buffers.at[ids, source, slots].set(rows)
    slice_width = FF // SPLIT

    def one_expert(args):
        expert, block = args
        inputs = block.reshape(N_EP * CAP, D)
        total = jnp.zeros((N_EP * CAP, D), jnp.float32)
        for part in range(SPLIT):
            start = (expert * FF + part * slice_width).astype(jnp.int32)
            w_gate = lax.dynamic_slice_in_dim(gate_weight, start, slice_width, 1)
            w_up = lax.dynamic_slice_in_dim(up_weight, start, slice_width, 1)
            w_down = lax.dynamic_slice_in_dim(down_weight, start, slice_width, 0)
            gate = jnp.dot(inputs, w_gate, preferred_element_type=jnp.float32)
            upper = jnp.dot(inputs, w_up, preferred_element_type=jnp.float32)
            hidden = (jax.nn.silu(gate) * upper).astype(jnp.bfloat16)
            partial_out = jnp.dot(hidden, w_down, preferred_element_type=jnp.float32).astype(jnp.bfloat16)
            total = total + partial_out.astype(jnp.float32)
        return total.reshape(N_EP, CAP, D)
    expert_out = lax.map(one_expert, (jnp.arange(EXPERTS, dtype=jnp.int32), buffers))
    picked = expert_out[ids, source, slots]
    mixed = lax.optimization_barrier(jnp.sum(mix_weights.reshape(N_EP, TOK_DEV, TOP, 1) * picked, axis=2))
    return mixed.reshape(TOKENS, D).astype(jnp.bfloat16)
```

```python
import functools

import jax
import jax.numpy as jnp
from jax import lax
from jax.experimental import pallas as pl
from jax.experimental.pallas import tpu as pltpu
from jax.sharding import PartitionSpec as P

TOP = 2
SPLIT = 4
FF_TILE = 256
OUT_TILE = 512
VMEM = pl.BlockSpec(memory_space=pltpu.VMEM)
SMEM = pl.BlockSpec(memory_space=pltpu.SMEM)


def places(ids, expert, capacity):
    tokens = ids.shape[1]
    named = ids[0:1] == expert
    for pick in range(1, TOP):
        named = named | (ids[pick : pick + 1] == expert)
    rows = lax.broadcasted_iota(jnp.int32, (tokens, tokens), 0)
    cols = lax.broadcasted_iota(jnp.int32, (tokens, tokens), 1)
    earlier = (rows < cols).astype(jnp.float32).astype(jnp.bfloat16)
    flags = jnp.broadcast_to(named.astype(jnp.float32), (8, tokens)).astype(jnp.bfloat16)
    slot = jnp.dot(flags, earlier, preferred_element_type=jnp.float32)[0:1].astype(jnp.int32)
    slot = jnp.where(named, slot, -1)
    places_of = lax.broadcasted_iota(jnp.int32, (capacity, tokens), 0)
    return (places_of == slot).astype(jnp.float32).astype(jnp.bfloat16)


def dispatch_kernel(experts, capacity, mine, ids, tokens, gain, *outs):
    values = tokens[...].astype(jnp.float32)
    scale = lax.rsqrt(jnp.mean(values * values, axis=-1, keepdims=True) + 1e-06)
    normed = (values * scale * gain[...]).astype(jnp.bfloat16)
    for shift in range(experts):
        onehot = places(ids[...], lax.rem(mine[0] + shift, experts), capacity)
        outs[shift][...] = jnp.dot(onehot, normed, preferred_element_type=jnp.float32).astype(
            jnp.bfloat16
        )


def combine_kernel(experts, capacity, mine, ids, mix, *refs):
    rets, out = refs[:experts], refs[experts]
    tokens = ids.shape[1]
    total = jnp.zeros(out.shape, jnp.float32)
    for shift in range(experts):
        expert = lax.rem(mine[0] + shift, experts)
        onehot = places(ids[...], expert, capacity)
        weight = jnp.zeros((1, tokens), jnp.float32)
        for pick in range(TOP):
            weight = weight + jnp.where(ids[pick : pick + 1] == expert, mix[pick : pick + 1], 0.0)
        column = jnp.transpose(jnp.broadcast_to(weight, (tokens, tokens)))[:, 0:1]
        rows = lax.dot_general(
            onehot, rets[shift][...], (((0,), (0,)), ((), ())), preferred_element_type=jnp.float32
        )
        total = total + column * rows
    out[...] = total.astype(out.dtype)


def ffn_kernel(*refs):
    xs, (gate_w, up_w, down_w), outs, (inputs, hidden) = (
        refs[:SPLIT],
        refs[SPLIT : SPLIT + 3],
        refs[SPLIT + 3 : 2 * SPLIT + 3],
        refs[2 * SPLIT + 3 :],
    )
    capacity = xs[0].shape[0]
    for i, block in enumerate(xs):
        inputs[i * capacity : (i + 1) * capacity] = block[...]

    @pl.loop(0, gate_w.shape[1] // FF_TILE)
    def _(j):
        cols = pl.ds(pl.multiple_of(j * FF_TILE, FF_TILE), FF_TILE)
        gate = jnp.dot(inputs[...], gate_w[:, cols], preferred_element_type=jnp.float32)
        upper = jnp.dot(inputs[...], up_w[:, cols], preferred_element_type=jnp.float32)
        hidden[:, cols] = (gate / (1.0 + jnp.exp(-gate)) * upper).astype(jnp.bfloat16)

    @pl.loop(0, down_w.shape[1] // OUT_TILE)
    def _(j):
        cols = pl.ds(pl.multiple_of(j * OUT_TILE, OUT_TILE), OUT_TILE)
        result = jnp.dot(hidden[...], down_w[:, cols], preferred_element_type=jnp.float32)
        for i, out in enumerate(outs):
            out[:, cols] = result[i * capacity : (i + 1) * capacity].astype(out.dtype)


def local(tokens, norm_gain, expert_ids, mix_weights, gate_weight, up_weight, down_weight):
    n_dev = lax.axis_size("ep")
    experts = n_dev // SPLIT
    tok_rows, width = tokens.shape
    ff = gate_weight.shape[1]
    capacity = SPLIT * ((tok_rows * TOP * SPLIT * 5 // (4 * n_dev) + SPLIT - 1) // SPLIT)
    mine = (lax.axis_index("ep") // SPLIT).astype(jnp.int32).reshape(1)
    ids = expert_ids.T
    mix = mix_weights.T
    block = jax.ShapeDtypeStruct((capacity, width), jnp.bfloat16)

    def across(array, shift):
        pairs = [
            (i, (i // SPLIT + shift) % experts * SPLIT + i % SPLIT) for i in range(n_dev)
        ]
        return lax.ppermute(array, "ep", pairs)

    def inside(array, flip):
        return lax.ppermute(array, "ep", [(i, i ^ flip) for i in range(n_dev)])

    sent = pl.pallas_call(
        functools.partial(dispatch_kernel, experts, capacity),
        out_shape=[block] * experts,
        in_specs=[SMEM, VMEM, VMEM, VMEM],
        out_specs=[VMEM] * experts,
        compiler_params=pltpu.CompilerParams(vmem_limit_bytes=12 * 2**20),
        cost_estimate=pl.CostEstimate(
            flops=2 * experts * capacity * tok_rows * width, bytes_accessed=4 * tok_rows * width, transcendentals=0
        ),
        name="dispatch",
    )(mine, ids, tokens, norm_gain.reshape(1, width))

    rows = SPLIT * capacity
    ffn = pl.pallas_call(
        ffn_kernel,
        out_shape=[block] * SPLIT,
        in_specs=[VMEM] * (SPLIT + 3),
        out_specs=[VMEM] * SPLIT,
        scratch_shapes=[
            pltpu.VMEM((rows, width), jnp.bfloat16),
            pltpu.VMEM((rows, ff), jnp.bfloat16),
        ],
        compiler_params=pltpu.CompilerParams(vmem_limit_bytes=40 * 2**20),
        cost_estimate=pl.CostEstimate(
            flops=6 * rows * width * ff, bytes_accessed=6 * width * ff, transcendentals=rows * ff
        ),
        name="ffn",
    )

    order = [0] + sorted(range(1, experts), key=lambda d: (-min(d, experts - d), d))
    arrived = {d: across(sent[d], d) if d else sent[d] for d in order}
    rets = [None] * experts
    for d in order:
        own = arrived[d]
        side = inside(own, 2)
        twin = inside(own, 1)
        twin_side = inside(side, 1)
        part, part_side, part_twin, part_twin_side = ffn(
            own, side, twin, twin_side, gate_weight, up_weight, down_weight
        )
        got_side = inside(part_twin_side, 1)
        got = inside(part_twin, 1)
        sum_side = (part_side.astype(jnp.float32) + got_side.astype(jnp.float32)).astype(jnp.bfloat16)
        got_far = inside(sum_side, 2)
        total = (
            part.astype(jnp.float32) + got.astype(jnp.float32) + got_far.astype(jnp.float32)
        ).astype(jnp.bfloat16)
        rets[d] = across(total, experts - d) if d else total

    return pl.pallas_call(
        functools.partial(combine_kernel, experts, capacity),
        out_shape=jax.ShapeDtypeStruct((tok_rows, width), jnp.bfloat16),
        in_specs=[SMEM, VMEM, VMEM] + [VMEM] * experts,
        out_specs=VMEM,
        compiler_params=pltpu.CompilerParams(vmem_limit_bytes=12 * 2**20),
        name="combine",
    )(mine, ids, mix, *rets)


def solution(mesh):
    in_specs = (
        P(("grp", "ep"), None),
        P(),
        P(("grp", "ep"), None),
        P(("grp", "ep"), None),
        P(None, "ep"),
        P(None, "ep"),
        P("ep", None),
    )
    out_specs = P(("grp", "ep"), None)
    return jax.shard_map(local, mesh=mesh, in_specs=in_specs, out_specs=out_specs, check_vma=False)
```

```python
import functools

import jax
import jax.numpy as jnp
from jax import lax
from jax.experimental import pallas as pl
from jax.experimental.pallas import tpu as pltpu
from jax.sharding import PartitionSpec as P


TOP = 2
SPLIT = 4
FF_TILE = 256
OUT_TILE = 512
VMEM = pl.BlockSpec(memory_space=pltpu.VMEM)
SMEM = pl.BlockSpec(memory_space=pltpu.SMEM)
HBM = pl.BlockSpec(memory_space=pltpu.HBM)


def places(ids, expert, capacity):
    tokens = ids.shape[1]
    named = ids[0:1] == expert
    for pick in range(1, TOP):
        named = named | (ids[pick : pick + 1] == expert)
    rows = lax.broadcasted_iota(jnp.int32, (tokens, tokens), 0)
    cols = lax.broadcasted_iota(jnp.int32, (tokens, tokens), 1)
    earlier = (rows < cols).astype(jnp.float32).astype(jnp.bfloat16)
    flags = jnp.broadcast_to(named.astype(jnp.float32), (8, tokens)).astype(jnp.bfloat16)
    slot = jnp.dot(flags, earlier, preferred_element_type=jnp.float32)[0:1].astype(jnp.int32)
    slot = jnp.where(named, slot, -1)
    places_of = lax.broadcasted_iota(jnp.int32, (capacity, tokens), 0)
    return (places_of == slot).astype(jnp.float32).astype(jnp.bfloat16)


def dispatch_kernel(experts, capacity, mine, ids, tokens, gain, *outs):
    values = tokens[...].astype(jnp.float32)
    scale = lax.rsqrt(jnp.mean(values * values, axis=-1, keepdims=True) + 1e-06)
    normed = (values * scale * gain[...]).astype(jnp.bfloat16)
    for shift in range(experts):
        onehot = places(ids[...], lax.rem(mine[0] + shift, experts), capacity)
        outs[shift][...] = jnp.dot(onehot, normed, preferred_element_type=jnp.float32).astype(
            jnp.bfloat16
        )


def combine_kernel(experts, capacity, mine, ids, mix, *refs):
    rets, out = refs[:experts], refs[experts]
    tokens = ids.shape[1]
    total = jnp.zeros(out.shape, jnp.float32)
    for shift in range(experts):
        expert = lax.rem(mine[0] + shift, experts)
        onehot = places(ids[...], expert, capacity)
        weight = jnp.zeros((1, tokens), jnp.float32)
        for pick in range(TOP):
            weight = weight + jnp.where(ids[pick : pick + 1] == expert, mix[pick : pick + 1], 0.0)
        column = jnp.transpose(jnp.broadcast_to(weight, (tokens, tokens)))[:, 0:1]
        rows = lax.dot_general(
            onehot, rets[shift][...], (((0,), (0,)), ((), ())), preferred_element_type=jnp.float32
        )
        total = total + column * rows
    out[...] = total.astype(out.dtype)


def load_kernel(*refs):
    count = len(refs) // 2
    copies = [
        pltpu.make_async_copy(refs[i], refs[count + i], refs[-1].at[i]) for i in range(count)
    ]
    for copy in copies:
        copy.start()
    for copy in copies:
        copy.wait()


def ffn_kernel(*refs):
    xs, (gate_w, up_w, down_w), outs, (inputs, hidden) = (
        refs[:SPLIT],
        refs[SPLIT : SPLIT + 3],
        refs[SPLIT + 3 : 2 * SPLIT + 3],
        refs[2 * SPLIT + 3 :],
    )
    capacity = xs[0].shape[0]
    for i, block in enumerate(xs):
        inputs[i * capacity : (i + 1) * capacity] = block[...]
    for start in range(0, gate_w.shape[1], FF_TILE):
        cols = pl.ds(start, FF_TILE)
        gate = jnp.dot(inputs[...], gate_w[:, cols], preferred_element_type=jnp.float32)
        upper = jnp.dot(inputs[...], up_w[:, cols], preferred_element_type=jnp.float32)
        hidden[:, cols] = (gate / (1.0 + jnp.exp(-gate)) * upper).astype(jnp.bfloat16)
    for start in range(0, down_w.shape[1], OUT_TILE):
        cols = pl.ds(start, OUT_TILE)
        result = jnp.dot(hidden[...], down_w[:, cols], preferred_element_type=jnp.float32)
        for i, out in enumerate(outs):
            out[:, cols] = result[i * capacity : (i + 1) * capacity].astype(out.dtype)


def shifts(experts):
    return [0] + sorted(range(1, experts), key=lambda d: (min(d, experts - d), d))


def local(tokens, norm_gain, expert_ids, mix_weights, gate_weight, up_weight, down_weight):
    n_dev = lax.axis_size("ep")
    experts = n_dev // SPLIT
    tok_rows, width = tokens.shape
    ff = gate_weight.shape[1]
    capacity = SPLIT * ((tok_rows * TOP * SPLIT * 5 // (4 * n_dev) + SPLIT - 1) // SPLIT)
    mine = (lax.axis_index("ep") // SPLIT).astype(jnp.int32).reshape(1)
    ids = expert_ids.T
    mix = mix_weights.T
    block = jax.ShapeDtypeStruct((capacity, width), jnp.bfloat16)

    def across(array, shift):
        pairs = [(i, (i // SPLIT + shift) % experts * SPLIT + i % SPLIT) for i in range(n_dev)]
        return lax.ppermute(array, "ep", pairs)

    def inside(array, flip):
        return lax.ppermute(array, "ep", [(i, i ^ flip) for i in range(n_dev)])

    def add(*parts):
        return sum(part.astype(jnp.float32) for part in parts).astype(jnp.bfloat16)

    sent = pl.pallas_call(
        functools.partial(dispatch_kernel, experts, capacity),
        out_shape=[block] * experts,
        in_specs=[SMEM, VMEM, VMEM, VMEM],
        out_specs=[VMEM] * experts,
        compiler_params=pltpu.CompilerParams(vmem_limit_bytes=8 * 2**20),
        cost_estimate=pl.CostEstimate(
            flops=2 * experts * capacity * tok_rows * width,
            bytes_accessed=4 * tok_rows * width,
            transcendentals=0,
        ),
        name="route",
    )(mine, ids, tokens, norm_gain.reshape(1, width))

    weights = (gate_weight, up_weight, down_weight)
    weights = pl.pallas_call(
        load_kernel,
        out_shape=[pltpu.VMEM(w.shape, w.dtype) for w in weights],
        in_specs=[HBM] * len(weights),
        out_specs=[VMEM] * len(weights),
        scratch_shapes=[pltpu.SemaphoreType.DMA((len(weights),))],
        compiler_params=pltpu.CompilerParams(vmem_limit_bytes=2**20),
        cost_estimate=pl.CostEstimate(
            flops=6 * 2**30, bytes_accessed=6 * width * ff, transcendentals=0
        ),
        name="fetch",
    )(*weights)

    rows = SPLIT * capacity
    ffn = pl.pallas_call(
        ffn_kernel,
        out_shape=[block] * SPLIT,
        in_specs=[VMEM] * (SPLIT + 3),
        out_specs=[VMEM] * SPLIT,
        scratch_shapes=[
            pltpu.VMEM((rows, width), jnp.bfloat16),
            pltpu.VMEM((rows, ff), jnp.bfloat16),
        ],
        compiler_params=pltpu.CompilerParams(vmem_limit_bytes=8 * 2**20),
        cost_estimate=pl.CostEstimate(
            flops=6 * rows * width * ff, bytes_accessed=6 * width * ff, transcendentals=rows * ff
        ),
        name="experts",
    )

    order = shifts(experts)
    arrived = {d: across(sent[d], d) if d else sent[d] for d in order}
    rets = [None] * experts
    for d in order:
        own = arrived[d]
        side = inside(own, 2)
        twin = inside(own, 1)
        twin_side = inside(side, 1)
        part, part_side, part_twin, part_twin_side = ffn(own, side, twin, twin_side, *weights)
        got_side = inside(part_twin_side, 1)
        got = inside(part_twin, 1)
        sum_side = add(part_side, got_side)
        got_far = inside(sum_side, 2)
        total = add(part, got, got_far)
        rets[d] = across(total, experts - d) if d else total

    return pl.pallas_call(
        functools.partial(combine_kernel, experts, capacity),
        out_shape=jax.ShapeDtypeStruct((tok_rows, width), jnp.bfloat16),
        in_specs=[SMEM, VMEM, VMEM] + [VMEM] * experts,
        out_specs=VMEM,
        compiler_params=pltpu.CompilerParams(vmem_limit_bytes=8 * 2**20),
        name="combine",
    )(mine, ids, mix, *rets)


def solution(mesh):
    in_specs = (
        P(("grp", "ep"), None),
        P(),
        P(("grp", "ep"), None),
        P(("grp", "ep"), None),
        P(None, "ep"),
        P(None, "ep"),
        P("ep", None),
    )
    out_specs = P(("grp", "ep"), None)
    return jax.shard_map(local, mesh=mesh, in_specs=in_specs, out_specs=out_specs, check_vma=False)
```

```python
import functools

import jax
import jax.numpy as jnp
from jax import lax
from jax.experimental import pallas as pl
from jax.experimental.pallas import tpu as pltpu
from jax.sharding import PartitionSpec as P


TOP = 2
SPLIT = 4
FF_TILE = 256
OUT_TILE = 512
VMEM = pl.BlockSpec(memory_space=pltpu.VMEM)
SMEM = pl.BlockSpec(memory_space=pltpu.SMEM)
EARLY = 1
LATE = (1, 0)
HBM = pl.BlockSpec(memory_space=pltpu.HBM)


def places(ids, expert, capacity):
    tokens = ids.shape[1]
    named = ids[0:1] == expert
    for pick in range(1, TOP):
        named = named | (ids[pick : pick + 1] == expert)
    rows = lax.broadcasted_iota(jnp.int32, (tokens, tokens), 0)
    cols = lax.broadcasted_iota(jnp.int32, (tokens, tokens), 1)
    earlier = (rows < cols).astype(jnp.float32).astype(jnp.bfloat16)
    flags = jnp.broadcast_to(named.astype(jnp.float32), (8, tokens)).astype(jnp.bfloat16)
    slot = jnp.dot(flags, earlier, preferred_element_type=jnp.float32)[0:1].astype(jnp.int32)
    slot = jnp.where(named, slot, -1)
    places_of = lax.broadcasted_iota(jnp.int32, (capacity, tokens), 0)
    return (places_of == slot).astype(jnp.float32).astype(jnp.bfloat16)


def dispatch_kernel(experts, capacity, mine, *refs):
    sources, outs, held, sem = refs[:3], refs[3 : 3 + experts], refs[3 + experts : -1], refs[-1]
    copies = [
        pltpu.make_async_copy(src, dst, sem.at[i]) for i, (src, dst) in enumerate(zip(sources, held))
    ]
    for copy in copies:
        copy.start()
    ids, tokens, gain = held
    copies[0].wait()
    onehots = [places(ids[...], lax.rem(mine[0] + d, experts), capacity) for d in range(experts)]
    for copy in copies[1:]:
        copy.wait()
    values = tokens[...].astype(jnp.float32)
    scale = lax.rsqrt(jnp.mean(values * values, axis=-1, keepdims=True) + 1e-06)
    normed = (values * scale * gain[...]).astype(jnp.bfloat16)
    for onehot, out in zip(onehots, outs):
        out[...] = jnp.dot(onehot, normed, preferred_element_type=jnp.float32).astype(jnp.bfloat16)


def combine_kernel(experts, capacity, chosen, last, mine, ids, mix, *refs):
    rets, refs = refs[: len(chosen)], refs[len(chosen) :]
    total = refs[0][...] if last else None
    out = refs[-1]
    tokens = ids.shape[1]
    for shift, ret in zip(chosen, rets):
        expert = lax.rem(mine[0] + shift, experts)
        onehot = places(ids[...], expert, capacity)
        weight = jnp.zeros((1, tokens), jnp.float32)
        for pick in range(TOP):
            weight = weight + jnp.where(ids[pick : pick + 1] == expert, mix[pick : pick + 1], 0.0)
        column = jnp.transpose(jnp.broadcast_to(weight, (tokens, tokens)))[:, 0:1]
        rows = lax.dot_general(
            onehot, ret[...], (((0,), (0,)), ((), ())), preferred_element_type=jnp.float32
        )
        total = column * rows if total is None else total + column * rows
    out[...] = total.astype(out.dtype)


def ffn_body(xs, weights, outs, inputs, hidden, ready):
    gate_w, up_w, down_w = weights
    capacity = xs[0].shape[0]
    for i, block in enumerate(xs):
        inputs[i * capacity : (i + 1) * capacity] = block[...]
    for start in range(0, gate_w.shape[1], FF_TILE):
        ready()
        cols = pl.ds(start, FF_TILE)
        gate = jnp.dot(inputs[...], gate_w[:, cols], preferred_element_type=jnp.float32)
        upper = jnp.dot(inputs[...], up_w[:, cols], preferred_element_type=jnp.float32)
        hidden[:, cols] = (gate / (1.0 + jnp.exp(-gate)) * upper).astype(jnp.bfloat16)
    for start in range(0, down_w.shape[1], OUT_TILE):
        ready()
        cols = pl.ds(start, OUT_TILE)
        result = jnp.dot(hidden[...], down_w[:, cols], preferred_element_type=jnp.float32)
        for i, out in enumerate(outs):
            out[:, cols] = result[i * capacity : (i + 1) * capacity].astype(out.dtype)


def ffn_kernel(count, *refs):
    xs, weights, outs = refs[:count], refs[count : count + 3], refs[count + 3 : 2 * count + 3]
    ffn_body(xs, weights, outs, refs[-2], refs[-1], lambda: None)


def first_ffn_kernel(count, *refs):
    xs, stored, refs = refs[:count], refs[count : count + 3], refs[count + 3 :]
    outs, weights, (inputs, hidden, sem) = refs[:count], refs[count : count + 3], refs[count + 3 :]
    groups = []
    for start in range(0, weights[0].shape[1], FF_TILE):
        groups.append([(k, pl.ds(start, FF_TILE)) for k in range(2)])
    for start in range(0, weights[2].shape[1], OUT_TILE):
        groups.append([(2, pl.ds(start, OUT_TILE))])
    copies, n = [], 0
    for group in groups:
        made = []
        for k, cols in group:
            made.append(
                pltpu.make_async_copy(stored[k].at[:, cols], weights[k].at[:, cols], sem.at[n])
            )
            n += 1
        copies.append(made)
    for made in copies:
        for copy in made:
            copy.start()
    left = iter(copies)

    def ready():
        for copy in next(left):
            copy.wait()

    ffn_body(xs, weights, outs, inputs, hidden, ready)


def shifts(experts):
    return [0] + sorted(range(1, experts), key=lambda d: (min(d, experts - d), d))


def local(tokens, norm_gain, expert_ids, mix_weights, gate_weight, up_weight, down_weight):
    n_dev = lax.axis_size("ep")
    experts = n_dev // SPLIT
    tok_rows, width = tokens.shape
    ff = gate_weight.shape[1]
    capacity = SPLIT * ((tok_rows * TOP * SPLIT * 5 // (4 * n_dev) + SPLIT - 1) // SPLIT)
    mine = (lax.axis_index("ep") // SPLIT).astype(jnp.int32).reshape(1)
    ids = expert_ids.T
    mix = mix_weights.T
    block = jax.ShapeDtypeStruct((capacity, width), jnp.bfloat16)

    def across(array, shift):
        pairs = [(i, (i // SPLIT + shift) % experts * SPLIT + i % SPLIT) for i in range(n_dev)]
        return lax.ppermute(array, "ep", pairs)

    def inside(array, flip):
        return lax.ppermute(array, "ep", [(i, i ^ flip) for i in range(n_dev)])

    def add(*parts):
        return sum(part.astype(jnp.float32) for part in parts).astype(jnp.bfloat16)

    inputs = (ids, tokens, norm_gain.reshape(1, width))
    sent = pl.pallas_call(
        functools.partial(dispatch_kernel, experts, capacity),
        out_shape=[block] * experts,
        in_specs=[SMEM, HBM, HBM, HBM],
        out_specs=[VMEM] * experts,
        scratch_shapes=[pltpu.VMEM(array.shape, array.dtype) for array in inputs]
        + [pltpu.SemaphoreType.DMA((len(inputs),))],
        compiler_params=pltpu.CompilerParams(vmem_limit_bytes=8 * 2**20),
        cost_estimate=pl.CostEstimate(
            flops=2 * experts * capacity * tok_rows * width,
            bytes_accessed=4 * tok_rows * width,
            transcendentals=0,
        ),
        name="route",
    )(mine, *(pltpu.with_memory_space_constraint(array, pltpu.HBM) for array in inputs))

    weights = (gate_weight, up_weight, down_weight)
    half = SPLIT // 2
    rows = half * capacity
    tiles = 2 * (ff // FF_TILE) + width // OUT_TILE
    scratch = [
        pltpu.VMEM((rows, width), jnp.bfloat16),
        pltpu.VMEM((rows, ff), jnp.bfloat16),
    ]
    shared = dict(
        compiler_params=pltpu.CompilerParams(vmem_limit_bytes=8 * 2**20),
        cost_estimate=pl.CostEstimate(
            flops=6 * rows * width * ff, bytes_accessed=6 * width * ff, transcendentals=rows * ff
        ),
        name="experts",
    )
    ffn = pl.pallas_call(
        functools.partial(ffn_kernel, half),
        out_shape=[block] * half,
        in_specs=[VMEM] * (half + 3),
        out_specs=[VMEM] * half,
        scratch_shapes=scratch,
        **shared,
    )
    first_ffn = pl.pallas_call(
        functools.partial(first_ffn_kernel, half),
        out_shape=[block] * half + [pltpu.VMEM(w.shape, w.dtype) for w in weights],
        in_specs=[VMEM] * half + [HBM] * 3,
        out_specs=[VMEM] * (half + 3),
        scratch_shapes=scratch + [pltpu.SemaphoreType.DMA((tiles,))],
        **shared,
    )

    order = shifts(experts)
    rets = [None] * experts
    for d in order:
        if d == 0:
            own = sent[0]
            side = inside(own, 2)
        elif d == EARLY:
            own = across(sent[d], d)
            side = across(inside(sent[d], 2), d)
        else:
            own = across(sent[d], d)
            side = inside(own, 2)
        twin = inside(own, 1)
        twin_side = inside(side, 1)
        if d == 0:
            kept = (pltpu.with_memory_space_constraint(w, pltpu.HBM) for w in weights)
            part, part_twin, *weights = first_ffn(own, twin, *kept)
        else:
            part, part_twin = ffn(own, twin, *weights)
        part_side, part_twin_side = ffn(side, twin_side, *weights)
        got_side = inside(part_twin_side, 1)
        got = inside(part_twin, 1)
        sum_side = add(part_side, got_side)
        got_far = inside(sum_side, 2)
        total = add(part, got, got_far)
        rets[d] = across(total, experts - d) if d else total

    def combine(chosen, dtype, *before):
        return pl.pallas_call(
            functools.partial(combine_kernel, experts, capacity, chosen, bool(before)),
            out_shape=jax.ShapeDtypeStruct((tok_rows, width), dtype),
            in_specs=[SMEM] + [VMEM] * (2 + len(chosen) + len(before)),
            out_specs=VMEM,
            compiler_params=pltpu.CompilerParams(vmem_limit_bytes=8 * 2**20),
            cost_estimate=pl.CostEstimate(
                flops=2 * len(chosen) * capacity * tok_rows * width,
                bytes_accessed=8 * tok_rows * width,
                transcendentals=0,
            ),
            name="combine",
        )(mine, ids, mix, *(rets[d] for d in chosen), *before)

    late = LATE if experts == 4 else tuple(order[-1:])
    early = combine(tuple(d for d in order if d not in late), jnp.float32)
    return combine(late, jnp.bfloat16, early)


def solution(mesh):
    in_specs = (
        P(("grp", "ep"), None),
        P(),
        P(("grp", "ep"), None),
        P(("grp", "ep"), None),
        P(None, "ep"),
        P(None, "ep"),
        P("ep", None),
    )
    out_specs = P(("grp", "ep"), None)
    return jax.shard_map(local, mesh=mesh, in_specs=in_specs, out_specs=out_specs, check_vma=False)
```

```python
import functools

import jax
import jax.numpy as jnp
from jax import lax
from jax.experimental import pallas as pl
from jax.experimental.pallas import tpu as pltpu
from jax.sharding import PartitionSpec as P


TOP = 2
SPLIT = 4
FF_TILE = 256
OUT_TILE = 512
VMEM = pl.BlockSpec(memory_space=pltpu.VMEM)
SMEM = pl.BlockSpec(memory_space=pltpu.SMEM)
EARLY = 1
LATE = (1, 0)
HBM = pl.BlockSpec(memory_space=pltpu.HBM)


def places(ids, expert, capacity):
    tokens = ids.shape[1]
    named = ids[0:1] == expert
    for pick in range(1, TOP):
        named = named | (ids[pick : pick + 1] == expert)
    rows = lax.broadcasted_iota(jnp.int32, (tokens, tokens), 0)
    cols = lax.broadcasted_iota(jnp.int32, (tokens, tokens), 1)
    earlier = (rows < cols).astype(jnp.float32).astype(jnp.bfloat16)
    flags = jnp.broadcast_to(named.astype(jnp.float32), (8, tokens)).astype(jnp.bfloat16)
    slot = jnp.dot(flags, earlier, preferred_element_type=jnp.float32)[0:1].astype(jnp.int32)
    slot = jnp.where(named, slot, -1)
    places_of = lax.broadcasted_iota(jnp.int32, (capacity, tokens), 0)
    return (places_of == slot).astype(jnp.float32).astype(jnp.bfloat16)


def dispatch_kernel(experts, capacity, mine, *refs):
    sources, outs, held, sem = refs[:3], refs[3 : 3 + experts], refs[3 + experts : -1], refs[-1]
    copies = [
        pltpu.make_async_copy(src, dst, sem.at[i]) for i, (src, dst) in enumerate(zip(sources, held))
    ]
    for copy in copies:
        copy.start()
    ids, tokens, gain = held
    copies[0].wait()
    onehots = [places(ids[...], lax.rem(mine[0] + d, experts), capacity) for d in range(experts)]
    for copy in copies[1:]:
        copy.wait()
    values = tokens[...].astype(jnp.float32)
    scale = lax.rsqrt(jnp.mean(values * values, axis=-1, keepdims=True) + 1e-06)
    normed = (values * scale * gain[...]).astype(jnp.bfloat16)
    for onehot, out in zip(onehots, outs):
        out[...] = jnp.dot(onehot, normed, preferred_element_type=jnp.float32).astype(jnp.bfloat16)


def table(experts, capacity, mine, ids, mix, shift):
    tokens = ids.shape[1]
    expert = lax.rem(mine[0] + shift, experts)
    weight = jnp.zeros((1, tokens), jnp.float32)
    for pick in range(TOP):
        weight = weight + jnp.where(ids[pick : pick + 1] == expert, mix[pick : pick + 1], 0.0)
    column = jnp.transpose(jnp.broadcast_to(weight, (tokens, tokens)))
    return places(ids[...], expert, capacity), column


def weighted(onehot, column, ret):
    rows = lax.dot_general(
        onehot, ret, (((0,), (0,)), ((), ())), preferred_element_type=jnp.float32
    )
    return column[:, 0:1] * rows


def early_kernel(experts, capacity, chosen, late, mine, ids, mix, *refs):
    rets, out, tables = refs[: len(chosen)], refs[len(chosen)], refs[len(chosen) + 1 :]
    total = None
    for shift, ret in zip(chosen, rets):
        part = weighted(*table(experts, capacity, mine, ids, mix, shift), ret[...])
        total = part if total is None else total + part
    out[...] = total
    for k, shift in enumerate(late):
        onehot, column = table(experts, capacity, mine, ids, mix, shift)
        tables[2 * k][...] = onehot
        tables[2 * k + 1][...] = column


def final_kernel(count, *refs):
    total, out = refs[0][...], refs[-1]
    for k in range(count):
        onehot, column, ret = (ref[...] for ref in refs[1 + 3 * k : 4 + 3 * k])
        total = total + weighted(onehot, column, ret)
    out[...] = total.astype(out.dtype)


def ffn_body(xs, weights, outs, inputs, hidden, ready):
    gate_w, up_w, down_w = weights
    capacity = xs[0].shape[0]
    for i, block in enumerate(xs):
        inputs[i * capacity : (i + 1) * capacity] = block[...]
    for start in range(0, gate_w.shape[1], FF_TILE):
        ready()
        cols = pl.ds(start, FF_TILE)
        gate = jnp.dot(inputs[...], gate_w[:, cols], preferred_element_type=jnp.float32)
        upper = jnp.dot(inputs[...], up_w[:, cols], preferred_element_type=jnp.float32)
        hidden[:, cols] = (gate / (1.0 + jnp.exp(-gate)) * upper).astype(jnp.bfloat16)
    for start in range(0, down_w.shape[1], OUT_TILE):
        ready()
        cols = pl.ds(start, OUT_TILE)
        result = jnp.dot(hidden[...], down_w[:, cols], preferred_element_type=jnp.float32)
        for i, out in enumerate(outs):
            out[:, cols] = result[i * capacity : (i + 1) * capacity].astype(out.dtype)


def ffn_kernel(count, *refs):
    xs, weights, outs = refs[:count], refs[count : count + 3], refs[count + 3 : 2 * count + 3]
    ffn_body(xs, weights, outs, refs[-2], refs[-1], lambda: None)


def first_ffn_kernel(count, *refs):
    xs, stored, refs = refs[:count], refs[count : count + 3], refs[count + 3 :]
    outs, weights, (inputs, hidden, sem) = refs[:count], refs[count : count + 3], refs[count + 3 :]
    groups = []
    for start in range(0, weights[0].shape[1], FF_TILE):
        groups.append([(k, pl.ds(start, FF_TILE)) for k in range(2)])
    for start in range(0, weights[2].shape[1], OUT_TILE):
        groups.append([(2, pl.ds(start, OUT_TILE))])
    copies, n = [], 0
    for group in groups:
        made = []
        for k, cols in group:
            made.append(
                pltpu.make_async_copy(stored[k].at[:, cols], weights[k].at[:, cols], sem.at[n])
            )
            n += 1
        copies.append(made)
    for made in copies:
        for copy in made:
            copy.start()
    left = iter(copies)

    def ready():
        for copy in next(left):
            copy.wait()

    ffn_body(xs, weights, outs, inputs, hidden, ready)


def shifts(experts):
    return [0] + sorted(range(1, experts), key=lambda d: (min(d, experts - d), d))


def local(tokens, norm_gain, expert_ids, mix_weights, gate_weight, up_weight, down_weight):
    n_dev = lax.axis_size("ep")
    experts = n_dev // SPLIT
    tok_rows, width = tokens.shape
    ff = gate_weight.shape[1]
    capacity = SPLIT * ((tok_rows * TOP * SPLIT * 5 // (4 * n_dev) + SPLIT - 1) // SPLIT)
    mine = (lax.axis_index("ep") // SPLIT).astype(jnp.int32).reshape(1)
    ids = expert_ids.T
    mix = mix_weights.T
    block = jax.ShapeDtypeStruct((capacity, width), jnp.bfloat16)

    def across(array, shift):
        pairs = [(i, (i // SPLIT + shift) % experts * SPLIT + i % SPLIT) for i in range(n_dev)]
        return lax.ppermute(array, "ep", pairs)

    def inside(array, flip):
        return lax.ppermute(array, "ep", [(i, i ^ flip) for i in range(n_dev)])

    def add(*parts):
        return sum(part.astype(jnp.float32) for part in parts).astype(jnp.bfloat16)

    inputs = (ids, tokens, norm_gain.reshape(1, width))
    sent = pl.pallas_call(
        functools.partial(dispatch_kernel, experts, capacity),
        out_shape=[block] * experts,
        in_specs=[SMEM, HBM, HBM, HBM],
        out_specs=[VMEM] * experts,
        scratch_shapes=[pltpu.VMEM(array.shape, array.dtype) for array in inputs]
        + [pltpu.SemaphoreType.DMA((len(inputs),))],
        compiler_params=pltpu.CompilerParams(vmem_limit_bytes=8 * 2**20),
        cost_estimate=pl.CostEstimate(
            flops=2 * experts * capacity * tok_rows * width,
            bytes_accessed=4 * tok_rows * width,
            transcendentals=0,
        ),
        name="route",
    )(mine, *(pltpu.with_memory_space_constraint(array, pltpu.HBM) for array in inputs))

    weights = (gate_weight, up_weight, down_weight)
    half = SPLIT // 2
    rows = half * capacity
    tiles = 2 * (ff // FF_TILE) + width // OUT_TILE
    scratch = [
        pltpu.VMEM((rows, width), jnp.bfloat16),
        pltpu.VMEM((rows, ff), jnp.bfloat16),
    ]
    shared = dict(
        compiler_params=pltpu.CompilerParams(vmem_limit_bytes=8 * 2**20),
        cost_estimate=pl.CostEstimate(
            flops=6 * rows * width * ff, bytes_accessed=6 * width * ff, transcendentals=rows * ff
        ),
        name="experts",
    )
    ffn = pl.pallas_call(
        functools.partial(ffn_kernel, half),
        out_shape=[block] * half,
        in_specs=[VMEM] * (half + 3),
        out_specs=[VMEM] * half,
        scratch_shapes=scratch,
        **shared,
    )
    first_ffn = pl.pallas_call(
        functools.partial(first_ffn_kernel, half),
        out_shape=[block] * half + [pltpu.VMEM(w.shape, w.dtype) for w in weights],
        in_specs=[VMEM] * half + [HBM] * 3,
        out_specs=[VMEM] * (half + 3),
        scratch_shapes=scratch + [pltpu.SemaphoreType.DMA((tiles,))],
        **shared,
    )

    order = shifts(experts)
    rets = [None] * experts
    for d in order:
        if d == 0:
            own = sent[0]
            side = inside(own, 2)
        elif d == EARLY:
            own = across(sent[d], d)
            side = across(inside(sent[d], 2), d)
        else:
            own = across(sent[d], d)
            side = inside(own, 2)
        twin = inside(own, 1)
        twin_side = inside(side, 1)
        if d == 0:
            kept = (pltpu.with_memory_space_constraint(w, pltpu.HBM) for w in weights)
            part, part_twin, *weights = first_ffn(own, twin, *kept)
        else:
            part, part_twin = ffn(own, twin, *weights)
        part_side, part_twin_side = ffn(side, twin_side, *weights)
        got_side = inside(part_twin_side, 1)
        got = inside(part_twin, 1)
        sum_side = add(part_side, got_side)
        got_far = inside(sum_side, 2)
        total = add(part, got, got_far)
        rets[d] = across(total, experts - d) if d else total

    late = LATE if experts == 4 else tuple(order[-1:])
    chosen = tuple(d for d in order if d not in late)
    tables = [
        jax.ShapeDtypeStruct((capacity, tok_rows), jnp.bfloat16),
        jax.ShapeDtypeStruct((tok_rows, tok_rows), jnp.float32),
    ]
    params = pltpu.CompilerParams(vmem_limit_bytes=8 * 2**20)
    total, *tables = pl.pallas_call(
        functools.partial(early_kernel, experts, capacity, chosen, late),
        out_shape=[jax.ShapeDtypeStruct((tok_rows, width), jnp.float32)] + tables * len(late),
        in_specs=[SMEM] + [VMEM] * (2 + len(chosen)),
        out_specs=[VMEM] * (1 + 2 * len(late)),
        compiler_params=params,
        name="combine",
    )(mine, ids, mix, *(rets[d] for d in chosen))
    last = [array for k, d in enumerate(late) for array in (*tables[2 * k : 2 * k + 2], rets[d])]
    return pl.pallas_call(
        functools.partial(final_kernel, len(late)),
        out_shape=jax.ShapeDtypeStruct((tok_rows, width), jnp.bfloat16),
        in_specs=[VMEM] * (1 + len(last)),
        out_specs=VMEM,
        compiler_params=params,
        name="finish",
    )(total, *last)


def solution(mesh):
    in_specs = (
        P(("grp", "ep"), None),
        P(),
        P(("grp", "ep"), None),
        P(("grp", "ep"), None),
        P(None, "ep"),
        P(None, "ep"),
        P("ep", None),
    )
    out_specs = P(("grp", "ep"), None)
    return jax.shard_map(local, mesh=mesh, in_specs=in_specs, out_specs=out_specs, check_vma=False)
```
